32 devices in a mesh: sp: 8 (over z, x), tp: 4 (over y, core).
Axes of the slice: x: 2, y: 2, z: 4, core: 2. Of those that a mesh axis runs over, the one named last changes fastest.
Arguments:
- x_resid: bfloat16 [1024, 2048], P(('sp', 'tp')), may hold values from -3 to 3
- query_proj: bfloat16 [1024, 2048], P('sp', 'tp'), may hold values from -6 to 6
- projected_key_heads: bfloat16 [1024, 1024], P('sp', 'tp'), may hold values from -6 to 6
- projected_value_heads: bfloat16 [1024, 1024], P('sp', 'tp'), may hold values from -6 to 6
- query_gain: float32 [128], replicated, may hold values from 1.3 to 6.5
- key_norm_gain: float32 [128], replicated, may hold values from 1.3 to 6.5
- out_weight: bfloat16 [2048, 2048], P('tp'), may hold values from -0.125 to 0.125
- ffn_gain: float32 [2048], replicated, may hold values from 0.1 to 1.9
- routing: int32 [1024, 2], P(('sp', 'tp')), may hold values from 0 to 7, all different within a row; in each aligned block of 32 rows (0 to 31, 32 to 63, ...) at most 16 rows name the same one
- route_scores: float32 [1024, 2], P(('sp', 'tp')), may hold values from -6 to 6
- expert_gate: bfloat16 [8, 2048, 4096], P('sp', None, 'tp'), may hold values from -0.125 to 0.125
- expert_up: bfloat16 [8, 2048, 4096], P('sp', None, 'tp'), may hold values from -0.125 to 0.125
- expert_down: bfloat16 [8, 4096, 2048], P('sp', 'tp'), may hold values from -0.09375 to 0.09375
Outputs:
- layer_out: bfloat16 [1024, 2048], P(('sp', 'tp'))
The draws below stay inside these ranges and needn't reach their ends.
Inputs may be any that keep to these rules, and one draw needn't show every extreme that they name: `routing`: each row names 2 different experts. In each aligned block of 32 rows (the rows of one device) no expert is named by more than 16 rows, a bound that some block reaches.
All inputs are finite; a program needn't handle non-finite values.
Results may differ from the reference program's by a relative error of at most 0.018.
The reference program's roundings to bfloat16 on the way count: a program that leaves them out, or rounds other values in their place, can miss the bound.
Values may be sent and summed in bfloat16 or wider, within the bound.
A program may use at most 128 MiB of HBM per device.

```python
import math
import jax
import jax.numpy as jnp
import numpy as np
from jax import lax

D = 2048
HEAD_WIDTH = 128
QUERY_HEADS = 16
KEY_VALUE_HEADS = 8
FF = 4096
TOP = 2
GRID_W = 64
TOK_DEV = 32
TOKEN_COUNT = 1024
EXPERTS = 8
CAP = 16
N_SP = 8
N_TP = 4


def draw_pair(key):
    base_key = jax.random.fold_in(key, 7)
    query_key, random_key_seed = jax.random.split(base_key, 2)
    query_rows = jax.random.normal(query_key, (TOKEN_COUNT, QUERY_HEADS, HEAD_WIDTH), jnp.float32)
    every_key_row = jax.random.normal(random_key_seed, (TOKEN_COUNT, KEY_VALUE_HEADS, HEAD_WIDTH), jnp.float32)
    query_rows = jnp.clip(query_rows, -6.0, 6.0)
    every_key_row = jnp.clip(every_key_row, -6.0, 6.0)
    return (query_rows.reshape(TOKEN_COUNT, QUERY_HEADS * HEAD_WIDTH), every_key_row.reshape(TOKEN_COUNT, KEY_VALUE_HEADS * HEAD_WIDTH))


def draw_query_proj(key, part):
    return draw_pair(key)[0].astype(jnp.bfloat16)


def draw_projected_key_heads(key, part):
    return draw_pair(key)[1].astype(jnp.bfloat16)


def draw_gains(key, salt):
    values = jax.random.uniform(jax.random.fold_in(key, salt), (HEAD_WIDTH,), jnp.float32)
    return 1.3 + 0.6 * values


def draw_query_gain(key, part):
    return draw_gains(key, 11)


def draw_key_norm_gain(key, part):
    return draw_gains(key, 13)


def block_scale(own_key, extent, cuts, smallest, high):
    level, own = 1.0, jax.random.fold_in(own_key, 6)
    for position, shards_of in cuts:
        steps = jnp.exp(jax.random.uniform(jax.random.fold_in(own, position), (shards_of,), jnp.float32, smallest / len(cuts), high / len(cuts)))
        level = level * jnp.repeat(steps, extent[position] // shards_of).reshape([-1 if axis == position else 1 for axis in range(len(extent))])
    return level


def assign_block(stream_key, own, number, rows, count, top, limit, skew):
    order = jax.random.permutation(stream_key, count)
    packed, common = load_shares(count, rows * top, limit, skew, True), load_shares(count, rows * top, limit, skew, False)
    places = jnp.arange(count)

    def named(sizes, offset_by):
        used = int((sizes > 0).sum())
        fixed = max(1, used // 4)
        shifted = fixed + (places - fixed + offset_by * (used - fixed)) % max(1, count - fixed)
        return jnp.zeros((count,), jnp.int32).at[order[jnp.where(places < fixed, places, shifted)]].set(jnp.asarray(sizes, jnp.int32))

    sizes = jnp.where(number % 4 == 0, named(packed, number // 4), named(common, number - number // 4 - 1))
    mixed = jax.random.permutation(jax.random.fold_in(own, 3), count)
    source_of, receiver = mixed[0:count // 2 * 2:2], mixed[1:count // 2 * 2:2]
    slack = jnp.minimum(sizes[source_of] - 1, limit - sizes[receiver]) // 2
    slack = jnp.where((source_of == order[0]) | (receiver == order[0]) | (sizes[receiver] == 0), 0, jnp.maximum(slack, 0))
    shifted = jax.random.randint(jax.random.fold_in(own, 4), (count // 2,), 0, 1 << 20) % (slack + 1)
    sizes = sizes.at[source_of].add(-shifted).at[receiver].add(shifted)
    items = jnp.searchsorted(jnp.cumsum(sizes), jnp.arange(rows * top), side="right").astype(jnp.int32)
    grid = items.reshape(top, rows).T
    grid = grid[jax.random.permutation(jax.random.fold_in(own, 1), rows)]
    offset_by = jax.random.randint(jax.random.fold_in(own, 2), (rows, 1), 0, top)
    return jnp.take_along_axis(grid, (jnp.arange(top)[None, :] + offset_by) % top, axis=1)


def load_shares(number_of, total, bound, slope, full):
    weights = [(1 << 20) // math.isqrt(rank ** slope) + 1 for rank in range(1, number_of + 1)]
    largest = bound if full else min(bound, max(-(-total // number_of), total * weights[0] // sum(weights)))
    least = 1 if total - largest >= number_of - 1 else 0
    given, rest = [largest] + [least] * (number_of - 1), total - largest - least * (number_of - 1)
    while rest > 0:
        movable = [i for i in range(1, number_of) if given[i] < largest] or [i for i in range(1, number_of) if given[i] < bound]
        whole, left = sum([weights[i] for i in movable]), rest
        for i in movable:
            addition = min(bound - given[i], max(1, left * weights[i] // whole), rest)
            given[i] = given[i] + addition
            rest = rest - addition
    return np.array(given)


def centred(stream_key, extent, scale, bound, shards=(), kind=jnp.bfloat16):
    loudness = block_scale(stream_key, extent, shards, -0.22, 0.18) if shards else 1.0
    drawn = jax.random.normal(stream_key, extent, jnp.float32) * scale * loudness
    return jnp.minimum(jnp.maximum(drawn, -bound), bound).astype(kind)


def setup_inputs(seed: int = 0) -> dict:
    key_of = jax.random.split(jax.random.key(seed), 14)
    x_resid = centred(key_of[0], (TOKEN_COUNT, D), 0.5, 3.0, ((0, 32),))
    query_proj = draw_query_proj(jax.random.fold_in(key_of[13], 71), 0)
    projected_key_heads = draw_projected_key_heads(jax.random.fold_in(key_of[13], 71), 0)
    projected_value_heads = centred(key_of[3], (TOKEN_COUNT, KEY_VALUE_HEADS * HEAD_WIDTH), 1.0, 6.0, ((0, 8), (1, 4)))
    query_gain = draw_query_gain(jax.random.fold_in(key_of[13], 71), 0)
    key_norm_gain = draw_key_norm_gain(jax.random.fold_in(key_of[13], 71), 0)
    out_weight = centred(key_of[6], (QUERY_HEADS * HEAD_WIDTH, D), (QUERY_HEADS * HEAD_WIDTH) ** -0.5, 0.125, ((0, 4),))
    ffn_gain = jnp.clip(1.0 + 0.18 * jax.random.normal(key_of[7], (D,), jnp.float32), 0.1, 1.9)
    routing_keys = jax.random.split(jax.random.fold_in(key_of[8], 1), TOKEN_COUNT // TOK_DEV)
    routing_turns = jax.random.permutation(jax.random.fold_in(key_of[8], 3), TOKEN_COUNT // TOK_DEV)
    routing = jax.vmap(lambda own, number: assign_block(jax.random.fold_in(key_of[8], 2), own, number, TOK_DEV, EXPERTS, TOP, CAP, 2))(routing_keys, routing_turns).reshape((TOKEN_COUNT, TOP))
    route_scores = centred(key_of[9], (TOKEN_COUNT, TOP), 1.5, 6.0, ((0, 32),), jnp.float32)
    expert_gate = centred(key_of[10], (EXPERTS, D, FF), D ** -0.5, 0.125, ((0, 8), (2, 4)))
    expert_up = centred(key_of[11], (EXPERTS, D, FF), D ** -0.5, 0.125, ((0, 8), (2, 4)))
    expert_down = centred(key_of[12], (EXPERTS, FF, D), FF ** -0.5, 0.09375, ((0, 8), (1, 4)))
    return {"x_resid": x_resid, "query_proj": query_proj, "projected_key_heads": projected_key_heads, "projected_value_heads": projected_value_heads, "query_gain": query_gain, "key_norm_gain": key_norm_gain, "out_weight": out_weight, "ffn_gain": ffn_gain, "routing": routing, "route_scores": route_scores, "expert_gate": expert_gate, "expert_up": expert_up, "expert_down": expert_down}


NORM_EPS = 1e-06
ROPE_BASE = 10000.0

def rms_scale(values, norm_gain):
    return values * lax.rsqrt(lax.optimization_barrier(jnp.mean(values * values, axis=-1, keepdims=True)) + NORM_EPS) * norm_gain

def grid_angles(token_positions, head_size):
    freq_count = head_size // 4
    frequency = ROPE_BASE ** (-jnp.arange(freq_count, dtype=jnp.float32) / freq_count)
    grid_row = (token_positions // GRID_W).astype(jnp.float32)
    grid_col = (token_positions % GRID_W).astype(jnp.float32)
    return (grid_row[:, None] * frequency, grid_col[:, None] * frequency)

def turn_half(values, angles):
    cosine = jnp.cos(angles)[:, None, :]
    sine_part = jnp.sin(angles)[:, None, :]
    leading, trailing = jnp.split(values, 2, axis=-1)
    return jnp.concatenate([leading * cosine - trailing * sine_part, trailing * cosine + leading * sine_part], axis=-1)

def normalize_rotate(projected, norm_gain, token_positions, heads):
    length = projected.shape[0]
    values = projected.astype(jnp.float32).reshape(length, heads, -1)
    head_size = values.shape[-1]
    values = rms_scale(values, norm_gain)
    row_angle, col_angle = grid_angles(token_positions, head_size)
    half_size = head_size // 2
    turned = jnp.concatenate([turn_half(values[..., :half_size], row_angle), turn_half(values[..., half_size:], col_angle)], axis=-1)
    return turned.reshape(length, heads * head_size).astype(jnp.bfloat16)

def reference(x_resid, query_proj, projected_key_heads, projected_value_heads, query_gain, key_norm_gain, out_weight, ffn_gain, routing, route_scores, expert_gate, expert_up, expert_down):
    token_positions = jnp.arange(TOKEN_COUNT, dtype=jnp.int32)
    query_rows = normalize_rotate(query_proj, query_gain, token_positions, QUERY_HEADS)
    rotated_key_rows = normalize_rotate(projected_key_heads, key_norm_gain, token_positions, KEY_VALUE_HEADS)
    head_groups = QUERY_HEADS // KEY_VALUE_HEADS
    rows_per_block = math.gcd(TOKEN_COUNT, 256)
    blocks_of_queries = query_rows.reshape(TOKEN_COUNT // rows_per_block, rows_per_block, KEY_VALUE_HEADS, head_groups, HEAD_WIDTH)
    grid_of_keys = rotated_key_rows.reshape(TOKEN_COUNT, KEY_VALUE_HEADS, HEAD_WIDTH).astype(jnp.float32)
    grid_of_values = projected_value_heads.reshape(TOKEN_COUNT, KEY_VALUE_HEADS, HEAD_WIDTH).astype(jnp.float32)

    def attend(query_block):
        scores = jnp.einsum('qhgd,khd->hgqk', query_block.astype(jnp.float32), grid_of_keys) * HEAD_WIDTH ** (-0.5)
        row_top = lax.optimization_barrier(jnp.max(scores, axis=-1, keepdims=True))
        weights = jnp.exp(scores - row_top)
        total = lax.optimization_barrier(jnp.sum(weights, axis=-1))
        rounded = lax.optimization_barrier(weights.astype(jnp.bfloat16)).astype(jnp.float32)
        summed = jnp.einsum('hgqk,khd->qhgd', rounded, grid_of_values)
        return (summed / jnp.transpose(total, (2, 0, 1))[..., None]).astype(jnp.bfloat16)
    attended = lax.map(attend, blocks_of_queries).reshape(TOKEN_COUNT, QUERY_HEADS * HEAD_WIDTH)
    col_width = QUERY_HEADS * HEAD_WIDTH // N_TP
    proj_sum = jnp.zeros((TOKEN_COUNT, D), jnp.float32)
    for block_index in range(N_TP):
        low_col = block_index * col_width
        partial_value = jnp.dot(attended[:, low_col:low_col + col_width], out_weight[low_col:low_col + col_width], preferred_element_type=jnp.float32)
        proj_sum = proj_sum + lax.optimization_barrier(partial_value.astype(jnp.bfloat16)).astype(jnp.float32)
    attn_proj = lax.optimization_barrier(proj_sum.astype(jnp.bfloat16)).astype(jnp.float32)
    middle = x_resid.astype(jnp.float32) + attn_proj
    normed = rms_scale(middle, ffn_gain).astype(jnp.bfloat16)
    flat_expert = routing.reshape(-1).astype(jnp.int32)
    assigned = flat_expert.shape[0]
    flat_token = jnp.arange(assigned, dtype=jnp.int32) // TOP
    flat_gate = jax.nn.softmax(route_scores.astype(jnp.float32), axis=-1).reshape(-1)
    sort_order = jnp.argsort(flat_expert, stable=True)
    sorted_token = flat_token[sort_order]
    sorted_gate = flat_gate[sort_order]
    counts = lax.optimization_barrier(jnp.sum((flat_expert[None, :] == jnp.arange(EXPERTS, dtype=jnp.int32)[:, None]).astype(jnp.int32), axis=1))
    starts = jnp.cumsum(counts) - counts
    most_rows = N_SP * N_TP * CAP
    slot_index = jnp.arange(most_rows, dtype=jnp.int32)
    hidden_width = FF // N_TP

    def run_expert(operands):
        gate_matrix, up_matrix, down_matrix, expert_index = operands
        filled = slot_index < counts[expert_index]
        where_rows = jnp.minimum(starts[expert_index] + slot_index, assigned - 1).astype(jnp.int32)
        token_ids = sorted_token[where_rows]
        inputs = normed[token_ids]
        gate_part = jnp.dot(inputs, gate_matrix, preferred_element_type=jnp.float32)
        up_part = jnp.dot(inputs, up_matrix, preferred_element_type=jnp.float32)
        hidden = (jax.nn.silu(gate_part) * up_part).astype(jnp.bfloat16)
        summed = jnp.zeros((most_rows, D), jnp.float32)
        for block_index in range(N_TP):
            low_row = block_index * hidden_width
            partial_value = jnp.dot(hidden[:, low_row:low_row + hidden_width], down_matrix[low_row:low_row + hidden_width], preferred_element_type=jnp.float32)
            summed = summed + lax.optimization_barrier(partial_value.astype(jnp.bfloat16)).astype(jnp.float32)
        expert_result = lax.optimization_barrier(summed.astype(jnp.bfloat16)).astype(jnp.float32)
        weight = jnp.where(filled, sorted_gate[where_rows], jnp.zeros((most_rows,), jnp.float32))
        targets = jnp.where(filled, token_ids, jnp.full((most_rows,), TOKEN_COUNT, jnp.int32))
        return (expert_result * weight[:, None], targets)
    contrib, targets = lax.map(run_expert, (expert_gate, expert_up, expert_down, jnp.arange(EXPERTS, dtype=jnp.int32)))
    routed = jax.ops.segment_sum(contrib.reshape(-1, D), targets.reshape(-1), num_segments=TOKEN_COUNT + 1)[:TOKEN_COUNT]
    return (middle + routed).astype(jnp.bfloat16)
```

```python
import functools
import math

import jax
import jax.numpy as jnp
import numpy as np
from jax import lax
from jax.experimental import pallas as pl
from jax.experimental.pallas import tpu as pltpu
from jax.sharding import PartitionSpec as P

MESH = pl.DeviceIdType.MESH

HEAD_WIDTH = 128
TOP = 2
GRID_W = 64


NORM_EPS = 1e-06
ROPE_BASE = 10000.0
NEG_LARGE = -1e30


def rms_scale(values, norm_gain):
    return (
        values * lax.rsqrt(jnp.mean(values * values, axis=-1, keepdims=True) + NORM_EPS) * norm_gain
    )


def grid_angles(token_positions, head_size):
    freq_count = head_size // 4
    frequency = ROPE_BASE ** (-jnp.arange(freq_count, dtype=jnp.float32) / freq_count)
    grid_row = (token_positions // GRID_W).astype(jnp.float32)
    grid_col = (token_positions % GRID_W).astype(jnp.float32)
    return (grid_row[:, None] * frequency, grid_col[:, None] * frequency)


def turn_half(values, angles):
    cosine = jnp.cos(angles)[:, None, :]
    sine_part = jnp.sin(angles)[:, None, :]
    leading, trailing = jnp.split(values, 2, axis=-1)
    return jnp.concatenate(
        [leading * cosine - trailing * sine_part, trailing * cosine + leading * sine_part], axis=-1
    )


def normalize_rotate(projected, norm_gain, token_positions, heads):
    length = projected.shape[0]
    values = projected.astype(jnp.float32).reshape(length, heads, -1)
    head_size = values.shape[-1]
    values = rms_scale(values, norm_gain)
    row_angle, col_angle = grid_angles(token_positions, head_size)
    half_size = head_size // 2
    turned = jnp.concatenate(
        [
            turn_half(values[..., :half_size], row_angle),
            turn_half(values[..., half_size:], col_angle),
        ],
        axis=-1,
    )
    return turned.reshape(length, heads * head_size).astype(jnp.bfloat16)


def local_plain(
    x_resid,
    query_proj,
    projected_key_heads,
    projected_value_heads,
    query_gain,
    key_norm_gain,
    out_weight,
    ffn_gain,
    routing,
    route_scores,
    expert_gate,
    expert_up,
    expert_down,
):
    seq_rows = query_proj.shape[0]
    q_heads = query_proj.shape[1] // HEAD_WIDTH
    kv_heads = projected_key_heads.shape[1] // HEAD_WIDTH
    head_groups = q_heads // kv_heads
    token_positions = lax.axis_index("sp") * seq_rows + jnp.arange(seq_rows, dtype=jnp.int32)
    query_rows = normalize_rotate(query_proj, query_gain, token_positions, q_heads)
    rotated_key_rows = normalize_rotate(
        projected_key_heads, key_norm_gain, token_positions, kv_heads
    )
    query_grid = query_rows.reshape(seq_rows, kv_heads, head_groups, HEAD_WIDTH)
    score_scale = HEAD_WIDTH ** (-0.5)
    run_max = jnp.full((kv_heads, head_groups, seq_rows), NEG_LARGE, jnp.float32)
    key_piece = lax.all_gather(rotated_key_rows, "sp", axis=0, tiled=True).reshape(
        -1, kv_heads, HEAD_WIDTH
    )
    value_piece = lax.all_gather(projected_value_heads, "sp", axis=0, tiled=True).reshape(
        -1, kv_heads, HEAD_WIDTH
    )
    scores = (
        jnp.einsum("qhgd,khd->hgqk", query_grid, key_piece, preferred_element_type=jnp.float32)
        * score_scale
    )
    new_max = jnp.maximum(run_max, jnp.max(scores, axis=-1))
    weights = jnp.exp(scores - new_max[..., None])
    new_total = jnp.sum(weights, axis=-1)
    addition = jnp.einsum(
        "hgqk,khd->hgqd",
        weights.astype(jnp.bfloat16),
        value_piece,
        preferred_element_type=jnp.float32,
    )
    attended = (
        (addition / new_total[..., None])
        .transpose(2, 0, 1, 3)
        .reshape(seq_rows, q_heads * HEAD_WIDTH)
        .astype(jnp.bfloat16)
    )
    own_tokens = x_resid.shape[0]
    model_width = x_resid.shape[1]
    row_block = attended
    attn_proj = lax.psum_scatter(
        jnp.dot(row_block, out_weight, preferred_element_type=jnp.float32).astype(jnp.bfloat16),
        "tp",
        scatter_dimension=0,
        tiled=True,
    )
    middle = x_resid.astype(jnp.float32) + attn_proj.astype(jnp.float32)
    normed = rms_scale(middle, ffn_gain).astype(jnp.bfloat16)
    experts_all = lax.axis_size("sp") * expert_gate.shape[0]
    capacity = max(2, 2 * own_tokens * TOP // experts_all)
    flat_expert = routing.reshape(-1)
    one_hot = (flat_expert[:, None] == jnp.arange(experts_all, dtype=jnp.int32)[None, :]).astype(
        jnp.int32
    )
    earlier = jnp.cumsum(one_hot, axis=0) - one_hot
    slot_rank = jnp.sum(earlier * one_hot, axis=1)
    target = flat_expert * capacity + slot_rank
    chooser = (
        jnp.arange(experts_all * capacity, dtype=jnp.int32)[:, None] == target[None, :]
    ).astype(jnp.float32)
    gate_share = jax.nn.softmax(route_scores, axis=-1).reshape(-1)
    picker = jnp.sum(chooser.reshape(experts_all * capacity, own_tokens, TOP), axis=2).astype(
        jnp.bfloat16
    )
    combiner = jnp.sum(
        (chooser * gate_share[None, :]).reshape(experts_all * capacity, own_tokens, TOP), axis=2
    )
    dispatch = (
        jnp.dot(picker, normed, preferred_element_type=jnp.float32)
        .astype(jnp.bfloat16)
        .reshape(experts_all, capacity, model_width)
    )
    gate_matrix = expert_gate[0]
    up_matrix = expert_up[0]
    down_matrix = expert_down[0]
    arrived = lax.all_to_all(dispatch, "sp", split_axis=0, concat_axis=0, tiled=True)
    row_block = lax.all_gather(arrived.reshape(-1, model_width), "tp", axis=0, tiled=True)
    gate_part = jnp.dot(row_block, gate_matrix, preferred_element_type=jnp.float32)
    up_part = jnp.dot(row_block, up_matrix, preferred_element_type=jnp.float32)
    hidden = (jax.nn.silu(gate_part) * up_part).astype(jnp.bfloat16)
    row_block = hidden
    expert_result = lax.psum_scatter(
        jnp.dot(row_block, down_matrix, preferred_element_type=jnp.float32).astype(jnp.bfloat16),
        "tp",
        scatter_dimension=0,
        tiled=True,
    )
    returned = lax.all_to_all(
        expert_result.reshape(-1, capacity, model_width),
        "sp",
        split_axis=0,
        concat_axis=0,
        tiled=True,
    )
    routed = jnp.einsum(
        "st,sd->td",
        combiner,
        returned.reshape(-1, model_width).astype(jnp.float32),
        precision=lax.Precision.HIGHEST,
    )
    return (middle + routed).astype(jnp.bfloat16)


def rdma(src, dst, send_sem, recv_sem, device):
    return pltpu.make_async_remote_copy(
        src_ref=src,
        dst_ref=dst,
        send_sem=send_sem,
        recv_sem=recv_sem,
        device_id=device,
        device_id_type=MESH,
    )


def turn_head(values, gain, cosine, sine):
    values = values * lax.rsqrt(jnp.mean(values * values, axis=-1, keepdims=True) + NORM_EPS) * gain
    width = values.shape[1]
    quarter = width // 4
    lane = lax.broadcasted_iota(jnp.int32, values.shape, 1)
    swapped = jnp.where(
        lane % (2 * quarter) < quarter,
        pltpu.roll(values, width - quarter, 1),
        pltpu.roll(values, quarter, 1),
    )
    return (values * cosine + swapped * sine).astype(jnp.bfloat16)


def flip(index, mask):
    bit = 1
    while bit <= mask:
        if mask // bit % 2:
            index = index + bit * (1 - 2 * (index // bit % 2))
        bit = bit * 2
    return index


def hop_order(count):
    half = count // 2
    near, far = list(range(2, half)), list(range(half, count))
    order = [0, 1, far.pop(0)]
    while near or far:
        for pool in (far, near, far):
            if pool:
                order.append(pool.pop(0))
    return order


def group_edges(count):
    return [0, 3 * count // 8, 6 * count // 8, count]


def layer_kernel(
    n_sp,
    n_tp,
    capacity,
    q_hbm,
    k_hbm,
    v_hbm,
    freq_hbm,
    qg_hbm,
    kg_hbm,
    x_hbm,
    fg_hbm,
    route_hbm,
    score_hbm,
    ow_hbm,
    wg_hbm,
    wu_hbm,
    wd_hbm,
    out_ref,
    q_ref,
    k_ref,
    freq_ref,
    qg_ref,
    kg_ref,
    x_ref,
    fg_ref,
    route_ref,
    score_ref,
    kbuf,
    vbuf,
    qs,
    att,
    part,
    prx,
    psum,
    rsbuf,
    direct,
    mid,
    disp,
    rows,
    hid,
    eo,
    cor,
    pair,
    yrec,
    res,
    ret,
    ow,
    wg,
    wu,
    wd,
    in_sem,
    w_sem,
    s_sem,
    k_r,
    v_r,
    a_r,
    rs_r,
    g_r,
    d_r,
    y_r,
    c_r,
    e_r,
    p_r,
    b_r,
):
    s = lax.axis_index("sp")
    t = lax.axis_index("tp")
    n_y = n_tp // 2
    y, c = t // 2, t % 2
    core_peer = (s, y * 2 + 1 - c)
    order = hop_order(n_sp)
    seq_rows, q_width = q_ref.shape
    kv_width = k_ref.shape[1]
    q_heads, kv_heads = q_width // HEAD_WIDTH, kv_width // HEAD_WIDTH
    groups = q_heads // kv_heads
    own, model = x_ref.shape
    f_width = wg.shape[1]
    tile = min(512, model)
    tiles = model // tile
    bits = [1 << i for i in range(n_sp.bit_length() - 1)]
    sent = [0] * 3
    edges = group_edges(n_sp)

    def send(stage, src, dst, recv_sem, device):
        rdma(src, dst, s_sem.at[stage], recv_sem, device).start()
        sent[stage] += math.prod(src.shape)

    def arrive(dst, recv_sem):
        rdma(dst, dst, recv_sem, recv_sem, core_peer).wait_recv()

    barrier = pltpu.get_barrier_semaphore()
    for bit in bits:
        pl.semaphore_signal(barrier, inc=1, device_id=(flip(s, bit), t), device_id_type=MESH)
    for d in range(1, n_tp):
        pl.semaphore_signal(barrier, inc=1, device_id=(s, (t + d) % n_tp), device_id_type=MESH)

    inputs = {}
    for name, src, dst in (
        ("k", k_hbm, k_ref),
        ("freq", freq_hbm, freq_ref),
        ("kg", kg_hbm, kg_ref),
        ("qg", qg_hbm, qg_ref),
        ("q", q_hbm, q_ref),
        ("route", route_hbm, route_ref),
        ("score", score_hbm, score_ref),
        ("x", x_hbm, x_ref),
        ("fg", fg_hbm, fg_ref),
    ):
        inputs[name] = pltpu.make_async_copy(src, dst, in_sem.at[len(inputs)])
        inputs[name].start()
    value_copies = []
    for h in range(kv_heads):
        cols = slice(h * HEAD_WIDTH, (h + 1) * HEAD_WIDTH)
        copy = pltpu.make_async_copy(
            v_hbm.at[:, cols], vbuf.at[h, 0], in_sem.at[len(inputs) + h]
        )
        copy.start()
        value_copies.append(copy)
    weight_copies = [
        pltpu.make_async_copy(ow_hbm, ow, w_sem.at[0]),
        pltpu.make_async_copy(wg_hbm.at[0], wg, w_sem.at[1]),
        pltpu.make_async_copy(wu_hbm.at[0], wu, w_sem.at[2]),
        pltpu.make_async_copy(wd_hbm.at[0], wd, w_sem.at[3]),
    ]

    table = (seq_rows, HEAD_WIDTH)
    place = lax.broadcasted_iota(jnp.int32, table, 0) + s * seq_rows
    column = lax.broadcasted_iota(jnp.int32, table, 1)
    step = jnp.where(column < HEAD_WIDTH // 2, place // GRID_W, place % GRID_W)
    inputs["freq"].wait()
    angles = step.astype(jnp.float32) * freq_ref[...]
    cosine, sine = jnp.cos(angles), jnp.sin(angles)
    sine = jnp.where(column % (HEAD_WIDTH // 2) < HEAD_WIDTH // 4, -sine, sine)
    inputs["kg"].wait()
    inputs["k"].wait()
    for h in range(kv_heads):
        cols = slice(h * HEAD_WIDTH, (h + 1) * HEAD_WIDTH)
        kbuf[h, 0] = turn_head(k_ref[:, cols].astype(jnp.float32), kg_ref[...], cosine, sine)
    pl.semaphore_wait(barrier, len(bits) + n_tp - 1)

    def hop_bit(kind, slot):
        return 2 if kind and slot == 3 else slot & -slot

    kinds = ((kbuf, k_r), (vbuf, v_r))

    def offer(kind, h, slot):
        buf, r_sem = kinds[kind]
        bit = hop_bit(kind, slot)
        send(0, buf.at[h, slot ^ bit], buf.at[h, slot], r_sem.at[h, slot], (flip(s, bit), t))

    settled = set()

    def got(kind, h, slot):
        if (kind, h, slot) not in settled:
            settled.add((kind, h, slot))
            buf, r_sem = kinds[kind]
            arrive(buf.at[h, slot], r_sem.at[h, slot])

    def pass_on(kind, h, slot):
        got(kind, h, slot)
        for child in range(n_sp - 1, slot, -1):
            if child ^ hop_bit(kind, child) == slot:
                offer(kind, h, child)

    for h in range(kv_heads):
        for bit in reversed(bits):
            offer(0, h, bit)
    for copy in value_copies:
        copy.wait()
    for bit in (bits[0], bits[-1]):
        for h in range(kv_heads):
            offer(1, h, bit)
    inputs["qg"].wait()
    inputs["q"].wait()
    for copy in weight_copies:
        copy.start()
    for h in range(q_heads):
        cols = slice(h * HEAD_WIDTH, (h + 1) * HEAD_WIDTH)
        kv, member = h // groups, h % groups
        qs[kv, member * seq_rows : (member + 1) * seq_rows, :] = turn_head(
            q_ref[:, cols].astype(jnp.float32), qg_ref[...], cosine, sine
        )
    inputs["route"].wait()
    inputs["score"].wait()
    total_slots = n_sp * capacity
    slot_at = lax.broadcasted_iota(jnp.int32, (total_slots, own), 0)
    slot_place = slot_at // capacity
    slot_expert = jnp.zeros_like(slot_at)
    for k, d in enumerate(order):
        slot_expert = jnp.where(slot_place == k, flip(s, d), slot_expert)
    first_hit = route_ref[0:1, :] == slot_expert
    named = first_hit | (route_ref[1:2, :] == slot_expert)
    earlier = (
        lax.broadcasted_iota(jnp.int32, (own, own), 0)
        < lax.broadcasted_iota(jnp.int32, (own, own), 1)
    )
    rank = jnp.dot(
        named.astype(jnp.float32).astype(jnp.bfloat16),
        earlier.astype(jnp.float32).astype(jnp.bfloat16),
        preferred_element_type=jnp.float32,
    )
    picked = jnp.where(
        named & (rank == (slot_at % capacity).astype(jnp.float32)), 1.0, 0.0
    )
    route_scores = score_ref[...]
    share = jnp.exp(route_scores - jnp.max(route_scores, axis=0, keepdims=True))
    share = share / jnp.sum(share, axis=0, keepdims=True)
    combiner = picked * jnp.where(first_hit, share[0:1, :], share[1:2, :])
    picker = picked.astype(jnp.bfloat16)

    singles = [bit for bit in reversed(bits) if bit > 1]
    deeper = [m for m in range(n_sp) if m % 2 == 0 and m & (m - 1)]
    for h in range(kv_heads):
        for bit in singles:
            pass_on(0, h, bit)
    for h in range(kv_heads):
        pass_on(1, h, bits[-1])
        for slot in deeper:
            pass_on(0, h, slot)
    for bit in bits[1:-1]:
        for h in range(kv_heads):
            offer(1, h, bit)
    for h in range(kv_heads):
        for slot in deeper:
            pass_on(1, h, slot)
    for h in range(kv_heads):
        pass_on(1, h, 1)
    keys_all = n_sp * seq_rows
    score_scale = HEAD_WIDTH ** (-0.5)
    heads_done = []
    for kv in range(kv_heads):
        for slot in range(1, n_sp):
            got(0, kv, slot)
        keys = kbuf[kv].reshape(keys_all, HEAD_WIDTH)
        scores = (
            lax.dot_general(
                qs[kv], keys, (((1,), (1,)), ((), ())), preferred_element_type=jnp.float32
            )
            * score_scale
        )
        weights = jnp.exp(scores - jnp.max(scores, axis=-1, keepdims=True))
        total = jnp.sum(weights, axis=-1, keepdims=True)
        heads_done.append((weights.astype(jnp.bfloat16), total))
    for kv in range(kv_heads):
        for slot in range(1, n_sp):
            got(1, kv, slot)
        values = vbuf[kv].reshape(keys_all, HEAD_WIDTH)
        weights, total = heads_done[kv]
        mixed = jnp.dot(weights, values, preferred_element_type=jnp.float32) / total
        for member in range(groups):
            h = kv * groups + member
            att[:, h * HEAD_WIDTH : (h + 1) * HEAD_WIDTH] = mixed[
                member * seq_rows : (member + 1) * seq_rows
            ].astype(jnp.bfloat16)

    weight_copies[0].wait()
    def project(cols):
        product = (
            jnp.dot(att[...], ow[:, cols], preferred_element_type=jnp.float32)
            .astype(jnp.bfloat16)
            .reshape(n_y, 2, own, -1)
        )
        for core in range(2):
            part[core, :, :, cols] = product[:, core]

    def swap(j):
        cols = slice(j * tile, (j + 1) * tile)
        send(0, part.at[1 - c, :, :, cols], prx.at[:, :, cols], a_r.at[j], core_peer)

    project(slice(0, tile))
    cols = slice(0, tile)
    for dy in range(1, n_y):
        far = (y + dy) % n_y
        for core in range(2):
            send(
                0,
                part.at[(c + core) % 2, far, :, cols],
                direct.at[dy, core, :, :],
                g_r.at[dy - 1, core],
                (s, far * 2 + (c + core) % 2),
            )
    project(slice(tile, model))
    for j in range(1, tiles):
        swap(j)
    swap(0)
    for j in range(1, tiles):
        cols = slice(j * tile, (j + 1) * tile)
        arrive(prx.at[:, :, cols], a_r.at[j])
        for dy in range(1, n_y):
            far = (y + dy) % n_y
            psum[dy, :, cols] = (
                part[c, far, :, cols].astype(jnp.float32) + prx[far, :, cols].astype(jnp.float32)
            ).astype(jnp.bfloat16)
            send(
                0,
                psum.at[dy, :, cols],
                rsbuf.at[dy, :, cols],
                rs_r.at[j, dy - 1],
                (s, far * 2 + c),
            )
    arrive(prx.at[:, :, slice(0, tile)], a_r.at[0])
    inputs["x"].wait()
    inputs["fg"].wait()
    squares = jnp.zeros((own, 1), jnp.float32)
    for j in range(tiles):
        cols = slice(j * tile, (j + 1) * tile)
        summed = part[c, y, :, cols].astype(jnp.float32) + prx[y, :, cols].astype(jnp.float32)
        for dy in range(1, n_y):
            if j:
                arrive(rsbuf.at[dy, :, cols], rs_r.at[j, dy - 1])
                summed = summed + rsbuf[dy, :, cols].astype(jnp.float32)
            else:
                for core in range(2):
                    arrive(direct.at[dy, core, :, :], g_r.at[dy - 1, core])
                    summed = summed + direct[dy, core].astype(jnp.float32)
        middle = x_ref[:, cols].astype(jnp.float32) + summed.astype(jnp.bfloat16).astype(jnp.float32)
        mid[:, cols] = middle
        squares = squares + jnp.sum(middle * middle, axis=-1, keepdims=True)
    normed = (mid[...] * lax.rsqrt(squares / model + NORM_EPS) * fg_ref[...]).astype(jnp.bfloat16)
    chosen = (
        jnp.dot(picker, normed, preferred_element_type=jnp.float32)
        .astype(jnp.bfloat16)
        .reshape(n_sp, capacity, model)
    )
    disp[...] = chosen

    def dispatch(k):
        send(disp.at[k], rows.at[k, t], d_s.at[k], rows_r.at[k, t], (flip(s, order[k]), t))

    def dispatch(k):
        send(1, disp.at[k], rows.at[k, c, y], d_r.at[k], (flip(s, order[k]), t))

    def forward(k):
        if k:
            arrive(rows.at[k, c, y], d_r.at[k])
        for dy in range(1, n_y):
            peer = ((y + dy) % n_y) * 2 + c
            send(1, rows.at[k, c, y], rows.at[k, c, y], y_r.at[k, dy - 1], (s, peer))
        swap_rows(k, y)

    def swap_rows(k, source):
        group = sum(k >= edge for edge in edges[1:-1])
        send(1, rows.at[k, c, source], rows.at[k, c, source], c_r.at[group], core_peer)

    def relay(k):
        for dy in range(1, n_y):
            source = (y + n_y - dy) % n_y
            arrive(rows.at[k, c, source], y_r.at[k, dy - 1])
            swap_rows(k, source)

    def settle(g):
        arrive(rows.at[edges[g] : edges[g + 1], 1 - c], c_r.at[g])

    def span(g, j):
        return slice(edges[g], edges[g + 1]), slice(j * tile, (j + 1) * tile)

    def give_pair(g, j):
        ks, cols = span(g, j)
        send(2, eo.at[1 - c, :, ks, :, cols], cor.at[:, ks, :, cols], e_r.at[g, j], core_peer)

    def sum_pair(g, j):
        ks, cols = span(g, j)
        arrive(cor.at[:, ks, :, cols], e_r.at[g, j])
        for dy in range(1, n_y):
            far = (y + dy) % n_y
            pair[dy, ks, :, cols] = (
                eo[c, far, ks, :, cols].astype(jnp.float32) + cor[far, ks, :, cols].astype(jnp.float32)
            ).astype(jnp.bfloat16)
            send(
                2,
                pair.at[dy, ks, :, cols],
                yrec.at[dy, ks, :, cols],
                p_r.at[g * tiles + j, dy - 1],
                (s, far * 2 + c),
            )

    def give_back(g, j):
        ks, cols = span(g, j)
        whole = eo[c, y, ks, :, cols].astype(jnp.float32) + cor[y, ks, :, cols].astype(jnp.float32)
        for dy in range(1, n_y):
            arrive(yrec.at[dy, ks, :, cols], p_r.at[g * tiles + j, dy - 1])
            whole = whole + yrec[dy, ks, :, cols].astype(jnp.float32)
        res[ks, :, cols] = whole.astype(jnp.bfloat16)
        for k in range(edges[g], edges[g + 1]):
            if k:
                send(
                    2, res.at[k, :, cols], ret.at[k, :, cols], b_r.at[j], (flip(s, order[k]), t)
                )

    def run(hooks, name):
        do(*hooks.get(name, ()))

    def experts(g, hooks):
        low, high = edges[g], edges[g + 1]
        group_rows = (high - low) * n_tp * capacity
        block = rows[low:high].reshape(group_rows, model)
        f_tile = min(256, f_width)
        for j in range(f_width // f_tile):
            cols = slice(j * f_tile, (j + 1) * f_tile)
            gate = jnp.dot(block, wg[:, cols], preferred_element_type=jnp.float32)
            up = jnp.dot(block, wu[:, cols], preferred_element_type=jnp.float32)
            hid[:group_rows, cols] = (gate / (1.0 + jnp.exp(-gate)) * up).astype(jnp.bfloat16)
            run(hooks, f"gu{g}{j}")
        if g == 0:
            weight_copies[3].wait()
        for j in range(tiles):
            cols = slice(j * tile, (j + 1) * tile)
            down = jnp.dot(hid[:group_rows, :], wd[:, cols], preferred_element_type=jnp.float32)
            down = down.astype(jnp.bfloat16).reshape(high - low, 2, n_y, capacity, tile)
            for core in range(2):
                for far in range(n_y):
                    eo[core, far, low:high, :, cols] = down[:, core, far]
            give_pair(g, j)
            run(hooks, f"dn{g}{j}")

    steps = {"D": dispatch, "F": forward, "R": relay, "S": settle, "P": sum_pair, "G": give_back}

    def do(*names):
        for name in names:
            steps[name[0]](*(int(d) for d in name[1:]))

    rows[0, c, y] = chosen[0]
    do("D2", "D3", "D1", "F0", "F1", "R0", "D4", "D5", "F2", "D6", "D7", "R1", "F3", "F4", "R2", "S0")
    weight_copies[1].wait()
    weight_copies[2].wait()
    experts(0, {"gu01": ("F5", "R4"), "gu03": ("R3", "F7"), "dn01": ("F6",), "dn02": ("P00", "R5"), "dn03": ("P01",)})
    do("S1")
    experts(1, {"gu10": ("P02", "P03"), "gu11": ("R7", "R6"), "gu13": ("G00",), "dn11": ("G01",), "dn12": ("P10",), "dn13": ("P11",)})
    do("S2")
    experts(2, {"gu20": ("P12", "P13", "G02", "G03"), "gu22": ("G10",), "dn20": ("G11",), "dn22": ("P20",), "dn23": ("P21", "G12")})
    do("P22", "P23", "G13", "G20", "G21", "G22", "G23")
    high = combiner.astype(jnp.bfloat16)
    rest = combiner - high.astype(jnp.float32)
    middle_part = rest.astype(jnp.bfloat16)
    low = (rest - middle_part.astype(jnp.float32)).astype(jnp.bfloat16)
    for j in range(tiles):
        cols = slice(j * tile, (j + 1) * tile)
        arrive(ret.at[1:, :, cols], b_r.at[j])
        returned = jnp.concatenate([res[0:1, :, cols], ret[1:, :, cols]]).reshape(total_slots, tile)
        routed = jnp.zeros((own, tile), jnp.float32)
        for piece in (high, middle_part, low):
            routed = routed + lax.dot_general(
                piece, returned, (((0,), (0,)), ((), ())), preferred_element_type=jnp.float32
            )
        out_ref[:, cols] = (mid[:, cols] + routed).astype(jnp.bfloat16)
    for stage, count in enumerate(sent):
        shipped = wg.at[pl.ds(0, count // f_width)]
        rdma(shipped, shipped, s_sem.at[stage], s_sem.at[stage], core_peer).wait_send()


def head_frequency():
    quarter = HEAD_WIDTH // 4
    frequency = ROPE_BASE ** (-np.arange(quarter, dtype=np.float32) / quarter)
    return jnp.asarray(np.tile(frequency, 4).reshape(1, HEAD_WIDTH), jnp.float32)


def local(
    x_resid,
    query_proj,
    projected_key_heads,
    projected_value_heads,
    query_gain,
    key_norm_gain,
    out_weight,
    ffn_gain,
    routing,
    route_scores,
    expert_gate,
    expert_up,
    expert_down,
):
    n_sp, n_tp = lax.axis_size("sp"), lax.axis_size("tp")
    own, model = x_resid.shape
    experts_all = n_sp * expert_gate.shape[0]
    capacity = max(2, 2 * own * TOP // experts_all)
    if capacity % 16 or n_tp & (n_tp - 1) or n_sp & (n_sp - 1) or n_tp < 2 or n_sp < 4 or expert_gate.shape[0] != 1:
        return local_plain(
            x_resid,
            query_proj,
            projected_key_heads,
            projected_value_heads,
            query_gain,
            key_norm_gain,
            out_weight,
            ffn_gain,
            routing,
            route_scores,
            expert_gate,
            expert_up,
            expert_down,
        )
    seq_rows, q_width = query_proj.shape
    kv_width = projected_key_heads.shape[1]
    kv_heads = kv_width // HEAD_WIDTH
    groups = q_width // kv_width
    f_width = expert_gate.shape[2]
    n_y = n_tp // 2
    tiles = model // min(512, model)
    edges = group_edges(n_sp)
    groups_all = len(edges) - 1
    group_most = max(b - a for a, b in zip(edges, edges[1:]))
    bf16 = jnp.bfloat16
    dma = pltpu.SemaphoreType.DMA
    hbm = pl.BlockSpec(memory_space=pl.ANY)
    return pl.pallas_call(
        functools.partial(layer_kernel, n_sp, n_tp, capacity),
        out_shape=pltpu.VMEM((own, model), bf16),
        in_specs=[hbm] * 14,
        out_specs=pl.BlockSpec(memory_space=pltpu.VMEM),
        scratch_shapes=[
            pltpu.VMEM(query_proj.shape, bf16),
            pltpu.VMEM(projected_key_heads.shape, bf16),
            pltpu.VMEM((1, HEAD_WIDTH), jnp.float32),
            pltpu.VMEM((1, HEAD_WIDTH), jnp.float32),
            pltpu.VMEM((1, HEAD_WIDTH), jnp.float32),
            pltpu.VMEM((own, model), bf16),
            pltpu.VMEM((1, model), jnp.float32),
            pltpu.VMEM((TOP, own), jnp.int32),
            pltpu.VMEM((TOP, own), jnp.float32),
            pltpu.VMEM((kv_heads, n_sp, seq_rows, HEAD_WIDTH), bf16),
            pltpu.VMEM((kv_heads, n_sp, seq_rows, HEAD_WIDTH), bf16),
            pltpu.VMEM((kv_heads, groups * seq_rows, HEAD_WIDTH), bf16),
            pltpu.VMEM((seq_rows, q_width), bf16),
            pltpu.VMEM((2, n_y, own, model), bf16),
            pltpu.VMEM((n_y, own, model), bf16),
            pltpu.VMEM((n_y, own, model), bf16),
            pltpu.VMEM((n_y, own, model), bf16),
            pltpu.VMEM((n_y, 2, own, model // tiles), bf16),
            pltpu.VMEM((own, model), jnp.float32),
            pltpu.VMEM((n_sp, capacity, model), bf16),
            pltpu.VMEM((n_sp, 2, n_y, capacity, model), bf16),
            pltpu.VMEM((group_most * n_tp * capacity, f_width), bf16),
            pltpu.VMEM((2, n_y, n_sp, capacity, model), bf16),
            pltpu.VMEM((n_y, n_sp, capacity, model), bf16),
            pltpu.VMEM((n_y, n_sp, capacity, model), bf16),
            pltpu.VMEM((n_y, n_sp, capacity, model), bf16),
            pltpu.VMEM((n_sp, capacity, model), bf16),
            pltpu.VMEM((n_sp, capacity, model), bf16),
            pltpu.VMEM(out_weight.shape, bf16),
            pltpu.VMEM(expert_gate.shape[1:], bf16),
            pltpu.VMEM(expert_up.shape[1:], bf16),
            pltpu.VMEM(expert_down.shape[1:], bf16),
            dma((9 + kv_heads,)),
            dma((4,)),
            dma((3,)),
            dma((kv_heads, n_sp)),
            dma((kv_heads, n_sp)),
            dma((tiles,)),
            dma((tiles, n_y - 1)),
            dma((n_y - 1, 2)),
            dma((n_sp,)),
            dma((n_sp, n_y - 1)),
            dma((groups_all,)),
            dma((groups_all, tiles)),
            dma((groups_all * tiles, n_y - 1)),
            dma((tiles,)),
        ],
        compiler_params=pltpu.CompilerParams(
            collective_id=0, has_side_effects=True, vmem_limit_bytes=56 * 1024 * 1024
        ),
    )(
        query_proj,
        projected_key_heads,
        projected_value_heads,
        head_frequency(),
        query_gain.reshape(1, -1),
        key_norm_gain.reshape(1, -1),
        x_resid,
        ffn_gain.reshape(1, -1),
        routing.T,
        route_scores.T,
        out_weight,
        expert_gate,
        expert_up,
        expert_down,
    )


def solution(mesh):
    in_specs = (
        P(("sp", "tp"), None),
        P("sp", "tp"),
        P("sp", "tp"),
        P("sp", "tp"),
        P(),
        P(),
        P("tp", None),
        P(),
        P(("sp", "tp"), None),
        P(("sp", "tp"), None),
        P("sp", None, "tp"),
        P("sp", None, "tp"),
        P("sp", "tp", None),
    )
    out_specs = P(("sp", "tp"), None)
    return jax.shard_map(local, mesh=mesh, in_specs=in_specs, out_specs=out_specs, check_vma=False)
```

```python
import functools
import math

import jax
import jax.numpy as jnp
import numpy as np
from jax import lax
from jax.experimental import pallas as pl
from jax.experimental.pallas import tpu as pltpu
from jax.sharding import PartitionSpec as P

MESH = pl.DeviceIdType.MESH

HEAD_WIDTH = 128
TOP = 2
GRID_W = 64


NORM_EPS = 1e-06
ROPE_BASE = 10000.0
NEG_LARGE = -1e30
PLAN_SPOTS = 8
PLAN_TILES = 4


def rms_scale(values, norm_gain):
    return (
        values * lax.rsqrt(jnp.mean(values * values, axis=-1, keepdims=True) + NORM_EPS) * norm_gain
    )


def grid_angles(token_positions, head_size):
    freq_count = head_size // 4
    frequency = ROPE_BASE ** (-jnp.arange(freq_count, dtype=jnp.float32) / freq_count)
    grid_row = (token_positions // GRID_W).astype(jnp.float32)
    grid_col = (token_positions % GRID_W).astype(jnp.float32)
    return (grid_row[:, None] * frequency, grid_col[:, None] * frequency)


def turn_half(values, angles):
    cosine = jnp.cos(angles)[:, None, :]
    sine_part = jnp.sin(angles)[:, None, :]
    leading, trailing = jnp.split(values, 2, axis=-1)
    return jnp.concatenate(
        [leading * cosine - trailing * sine_part, trailing * cosine + leading * sine_part], axis=-1
    )


def normalize_rotate(projected, norm_gain, token_positions, heads):
    length = projected.shape[0]
    values = projected.astype(jnp.float32).reshape(length, heads, -1)
    head_size = values.shape[-1]
    values = rms_scale(values, norm_gain)
    row_angle, col_angle = grid_angles(token_positions, head_size)
    half_size = head_size // 2
    turned = jnp.concatenate(
        [
            turn_half(values[..., :half_size], row_angle),
            turn_half(values[..., half_size:], col_angle),
        ],
        axis=-1,
    )
    return turned.reshape(length, heads * head_size).astype(jnp.bfloat16)


def local_plain(
    x_resid,
    query_proj,
    projected_key_heads,
    projected_value_heads,
    query_gain,
    key_norm_gain,
    out_weight,
    ffn_gain,
    routing,
    route_scores,
    expert_gate,
    expert_up,
    expert_down,
):
    seq_rows = query_proj.shape[0]
    q_heads = query_proj.shape[1] // HEAD_WIDTH
    kv_heads = projected_key_heads.shape[1] // HEAD_WIDTH
    head_groups = q_heads // kv_heads
    token_positions = lax.axis_index("sp") * seq_rows + jnp.arange(seq_rows, dtype=jnp.int32)
    query_rows = normalize_rotate(query_proj, query_gain, token_positions, q_heads)
    rotated_key_rows = normalize_rotate(
        projected_key_heads, key_norm_gain, token_positions, kv_heads
    )
    query_grid = query_rows.reshape(seq_rows, kv_heads, head_groups, HEAD_WIDTH)
    score_scale = HEAD_WIDTH ** (-0.5)
    run_max = jnp.full((kv_heads, head_groups, seq_rows), NEG_LARGE, jnp.float32)
    key_piece = lax.all_gather(rotated_key_rows, "sp", axis=0, tiled=True).reshape(
        -1, kv_heads, HEAD_WIDTH
    )
    value_piece = lax.all_gather(projected_value_heads, "sp", axis=0, tiled=True).reshape(
        -1, kv_heads, HEAD_WIDTH
    )
    scores = (
        jnp.einsum("qhgd,khd->hgqk", query_grid, key_piece, preferred_element_type=jnp.float32)
        * score_scale
    )
    new_max = jnp.maximum(run_max, jnp.max(scores, axis=-1))
    weights = jnp.exp(scores - new_max[..., None])
    new_total = jnp.sum(weights, axis=-1)
    addition = jnp.einsum(
        "hgqk,khd->hgqd",
        weights.astype(jnp.bfloat16),
        value_piece,
        preferred_element_type=jnp.float32,
    )
    attended = (
        (addition / new_total[..., None])
        .transpose(2, 0, 1, 3)
        .reshape(seq_rows, q_heads * HEAD_WIDTH)
        .astype(jnp.bfloat16)
    )
    own_tokens = x_resid.shape[0]
    model_width = x_resid.shape[1]
    row_block = attended
    attn_proj = lax.psum_scatter(
        jnp.dot(row_block, out_weight, preferred_element_type=jnp.float32).astype(jnp.bfloat16),
        "tp",
        scatter_dimension=0,
        tiled=True,
    )
    middle = x_resid.astype(jnp.float32) + attn_proj.astype(jnp.float32)
    normed = rms_scale(middle, ffn_gain).astype(jnp.bfloat16)
    experts_all = lax.axis_size("sp") * expert_gate.shape[0]
    capacity = max(2, 2 * own_tokens * TOP // experts_all)
    flat_expert = routing.reshape(-1)
    one_hot = (flat_expert[:, None] == jnp.arange(experts_all, dtype=jnp.int32)[None, :]).astype(
        jnp.int32
    )
    earlier = jnp.cumsum(one_hot, axis=0) - one_hot
    slot_rank = jnp.sum(earlier * one_hot, axis=1)
    target = flat_expert * capacity + slot_rank
    chooser = (
        jnp.arange(experts_all * capacity, dtype=jnp.int32)[:, None] == target[None, :]
    ).astype(jnp.float32)
    gate_share = jax.nn.softmax(route_scores, axis=-1).reshape(-1)
    picker = jnp.sum(chooser.reshape(experts_all * capacity, own_tokens, TOP), axis=2).astype(
        jnp.bfloat16
    )
    combiner = jnp.sum(
        (chooser * gate_share[None, :]).reshape(experts_all * capacity, own_tokens, TOP), axis=2
    )
    dispatch = (
        jnp.dot(picker, normed, preferred_element_type=jnp.float32)
        .astype(jnp.bfloat16)
        .reshape(experts_all, capacity, model_width)
    )
    gate_matrix = expert_gate[0]
    up_matrix = expert_up[0]
    down_matrix = expert_down[0]
    arrived = lax.all_to_all(dispatch, "sp", split_axis=0, concat_axis=0, tiled=True)
    row_block = lax.all_gather(arrived.reshape(-1, model_width), "tp", axis=0, tiled=True)
    gate_part = jnp.dot(row_block, gate_matrix, preferred_element_type=jnp.float32)
    up_part = jnp.dot(row_block, up_matrix, preferred_element_type=jnp.float32)
    hidden = (jax.nn.silu(gate_part) * up_part).astype(jnp.bfloat16)
    row_block = hidden
    expert_result = lax.psum_scatter(
        jnp.dot(row_block, down_matrix, preferred_element_type=jnp.float32).astype(jnp.bfloat16),
        "tp",
        scatter_dimension=0,
        tiled=True,
    )
    returned = lax.all_to_all(
        expert_result.reshape(-1, capacity, model_width),
        "sp",
        split_axis=0,
        concat_axis=0,
        tiled=True,
    )
    routed = jnp.einsum(
        "st,sd->td",
        combiner,
        returned.reshape(-1, model_width).astype(jnp.float32),
        precision=lax.Precision.HIGHEST,
    )
    return (middle + routed).astype(jnp.bfloat16)


def rdma(src, dst, send_sem, recv_sem, device):
    return pltpu.make_async_remote_copy(
        src_ref=src,
        dst_ref=dst,
        send_sem=send_sem,
        recv_sem=recv_sem,
        device_id=device,
        device_id_type=MESH,
    )


def turn_head(values, gain, cosine, sine):
    values = values * lax.rsqrt(jnp.mean(values * values, axis=-1, keepdims=True) + NORM_EPS) * gain
    width = values.shape[1]
    quarter = width // 4
    lane = lax.broadcasted_iota(jnp.int32, values.shape, 1)
    swapped = jnp.where(
        lane % (2 * quarter) < quarter,
        pltpu.roll(values, width - quarter, 1),
        pltpu.roll(values, quarter, 1),
    )
    return (values * cosine + swapped * sine).astype(jnp.bfloat16)


def flip(index, mask):
    bit = 1
    while bit <= mask:
        if mask // bit % 2:
            index = index + bit * (1 - 2 * (index // bit % 2))
        bit = bit * 2
    return index


def hop_order(count):
    half, quarter = count // 2, count // 4
    near, far = list(range(quarter, half)), list(range(half, count))
    far = far[1:] + far[:1]
    order = list(range(quarter)) + [far.pop(0)]
    while near or far:
        for pool in (far, near, far):
            if pool:
                order.append(pool.pop(0))
    return order


def hop_bit(kind, slot):
    return {3: 2, 6: 6}.get(slot, slot & -slot) if kind else slot & -slot


def inner_slots(count, kind):
    parents = {child ^ hop_bit(kind, child) for child in range(1, count)}
    return sorted(parents - {0})


def crossed_first(count):
    return [k for k, hop in enumerate(hop_order(count)) if count // 4 <= hop < count // 2]


def group_edges(count):
    return [0, 3 * count // 8, 6 * count // 8, count]


def layer_kernel(
    n_sp,
    n_tp,
    capacity,
    q_hbm,
    k_hbm,
    v_hbm,
    freq_hbm,
    qg_hbm,
    kg_hbm,
    x_hbm,
    fg_hbm,
    route_hbm,
    score_hbm,
    ow_hbm,
    wg_hbm,
    wu_hbm,
    wd_hbm,
    out_ref,
    q_ref,
    k_ref,
    freq_ref,
    qg_ref,
    kg_ref,
    x_ref,
    fg_ref,
    route_ref,
    score_ref,
    kbuf,
    vbuf,
    qs,
    att,
    part,
    prx,
    psum,
    rsbuf,
    direct,
    mid,
    disp,
    via,
    rows,
    hid,
    eo,
    cor,
    pair,
    yrec,
    res,
    ret,
    ow,
    wg,
    wu,
    wd,
    in_sem,
    w_sem,
    s_sem,
    k_r,
    v_r,
    a_r,
    rs_r,
    g_r,
    d_r,
    v2_r,
    y_r,
    c_r,
    e_r,
    p_r,
    b_r,
):
    s = lax.axis_index("sp")
    t = lax.axis_index("tp")
    n_y = n_tp // 2
    y, c = t // 2, t % 2
    core_peer = (s, y * 2 + 1 - c)
    order = hop_order(n_sp)
    seq_rows, q_width = q_ref.shape
    kv_width = k_ref.shape[1]
    q_heads, kv_heads = q_width // HEAD_WIDTH, kv_width // HEAD_WIDTH
    groups = q_heads // kv_heads
    own, model = x_ref.shape
    f_width = wg.shape[1]
    tile = min(512, model)
    tiles = model // tile
    bits = [1 << i for i in range(n_sp.bit_length() - 1)]
    sent = [0] * 3
    edges = group_edges(n_sp)
    crossed = crossed_first(n_sp)

    def send(stage, src, dst, recv_sem, device):
        rdma(src, dst, s_sem.at[stage], recv_sem, device).start()
        sent[stage] += math.prod(src.shape)

    def arrive(dst, recv_sem):
        rdma(dst, dst, recv_sem, recv_sem, core_peer).wait_recv()

    barrier = pltpu.get_barrier_semaphore()
    for bit in bits:
        pl.semaphore_signal(barrier, inc=1, device_id=(flip(s, bit), t), device_id_type=MESH)
    for d in range(1, n_tp):
        pl.semaphore_signal(barrier, inc=1, device_id=(s, (t + d) % n_tp), device_id_type=MESH)

    inputs = {}
    for name, src, dst in (
        ("k", k_hbm, k_ref),
        ("freq", freq_hbm, freq_ref),
        ("kg", kg_hbm, kg_ref),
        ("qg", qg_hbm, qg_ref),
        ("q", q_hbm, q_ref),
        ("route", route_hbm, route_ref),
        ("score", score_hbm, score_ref),
        ("x", x_hbm, x_ref),
        ("fg", fg_hbm, fg_ref),
    ):
        inputs[name] = pltpu.make_async_copy(src, dst, in_sem.at[len(inputs)])
        inputs[name].start()
    value_copies = []
    for h in range(kv_heads):
        cols = slice(h * HEAD_WIDTH, (h + 1) * HEAD_WIDTH)
        copy = pltpu.make_async_copy(
            v_hbm.at[:, cols], vbuf.at[h, 0], in_sem.at[len(inputs) + h]
        )
        copy.start()
        value_copies.append(copy)
    weight_copies = [
        pltpu.make_async_copy(ow_hbm, ow, w_sem.at[0]),
        pltpu.make_async_copy(wg_hbm.at[0], wg, w_sem.at[1]),
        pltpu.make_async_copy(wu_hbm.at[0], wu, w_sem.at[2]),
        pltpu.make_async_copy(wd_hbm.at[0], wd, w_sem.at[3]),
    ]

    table = (seq_rows, HEAD_WIDTH)
    place = lax.broadcasted_iota(jnp.int32, table, 0) + s * seq_rows
    column = lax.broadcasted_iota(jnp.int32, table, 1)
    step = jnp.where(column < HEAD_WIDTH // 2, place // GRID_W, place % GRID_W)
    inputs["freq"].wait()
    angles = step.astype(jnp.float32) * freq_ref[...]
    cosine, sine = jnp.cos(angles), jnp.sin(angles)
    sine = jnp.where(column % (HEAD_WIDTH // 2) < HEAD_WIDTH // 4, -sine, sine)
    inputs["kg"].wait()
    inputs["k"].wait()
    for h in range(kv_heads):
        cols = slice(h * HEAD_WIDTH, (h + 1) * HEAD_WIDTH)
        kbuf[h, 0] = turn_head(k_ref[:, cols].astype(jnp.float32), kg_ref[...], cosine, sine)
    pl.semaphore_wait(barrier, len(bits) + n_tp - 1)

    kinds = ((kbuf, k_r), (vbuf, v_r))

    def offer(kind, h, slot):
        buf, r_sem = kinds[kind]
        bit = hop_bit(kind, slot)
        spot = inner[kind].index(slot) if slot in inner[kind] else len(inner[kind])
        send(0, buf.at[h, slot ^ bit], buf.at[h, slot], r_sem.at[h, spot], (flip(s, bit), t))

    inner = [inner_slots(n_sp, kind) for kind in range(2)]
    settled = set()

    def got(kind, h, slot):
        if (kind, h, slot) not in settled:
            settled.add((kind, h, slot))
            buf, r_sem = kinds[kind]
            arrive(buf.at[h, slot], r_sem.at[h, inner[kind].index(slot)])

    def got_all(kind, h):
        buf, r_sem = kinds[kind]
        for slot in inner[kind]:
            got(kind, h, slot)
        arrive(buf.at[h, pl.ds(0, n_sp - 1 - len(inner[kind]))], r_sem.at[h, len(inner[kind])])

    def pass_on(kind, h, slot):
        got(kind, h, slot)
        for child in range(n_sp - 1, slot, -1):
            if child ^ hop_bit(kind, child) == slot:
                offer(kind, h, child)

    for h in range(kv_heads):
        for bit in reversed(bits):
            offer(0, h, bit)
    for copy in value_copies:
        copy.wait()
    for bit in (bits[0], bits[-1]):
        for h in range(kv_heads):
            offer(1, h, bit)
    inputs["qg"].wait()
    inputs["q"].wait()
    for copy in weight_copies:
        copy.start()
    for h in range(q_heads):
        cols = slice(h * HEAD_WIDTH, (h + 1) * HEAD_WIDTH)
        kv, member = h // groups, h % groups
        qs[kv, member * seq_rows : (member + 1) * seq_rows, :] = turn_head(
            q_ref[:, cols].astype(jnp.float32), qg_ref[...], cosine, sine
        )
    inputs["route"].wait()
    inputs["score"].wait()
    total_slots = n_sp * capacity
    slot_at = lax.broadcasted_iota(jnp.int32, (total_slots, own), 0)
    slot_place = slot_at // capacity
    slot_expert = jnp.zeros_like(slot_at)
    for k, d in enumerate(order):
        slot_expert = jnp.where(slot_place == k, flip(s, d), slot_expert)
    first_hit = route_ref[0:1, :] == slot_expert
    named = first_hit | (route_ref[1:2, :] == slot_expert)
    earlier = (
        lax.broadcasted_iota(jnp.int32, (own, own), 0)
        < lax.broadcasted_iota(jnp.int32, (own, own), 1)
    )
    rank = jnp.dot(
        named.astype(jnp.float32).astype(jnp.bfloat16),
        earlier.astype(jnp.float32).astype(jnp.bfloat16),
        preferred_element_type=jnp.float32,
    )
    picked = jnp.where(
        named & (rank == (slot_at % capacity).astype(jnp.float32)), 1.0, 0.0
    )
    route_scores = score_ref[...]
    share = jnp.exp(route_scores - jnp.max(route_scores, axis=0, keepdims=True))
    share = share / jnp.sum(share, axis=0, keepdims=True)
    combiner = picked * jnp.where(first_hit, share[0:1, :], share[1:2, :])
    picker = picked.astype(jnp.bfloat16)

    singles = [bit for bit in reversed(bits) if bit > 1]
    deeper = [m for m in range(n_sp) if m % 2 == 0 and m & (m - 1)]
    for h in range(kv_heads):
        for bit in singles:
            pass_on(0, h, bit)
        for slot in deeper:
            offer(1, h, slot)
    for h in range(kv_heads):
        if h == 0:
            for bit in bits[1:-1]:
                offer(1, h, bit)
        pass_on(1, h, bits[-1])
        pass_on(1, h, 1)
        for slot in deeper:
            pass_on(0, h, slot)
        if h:
            for bit in bits[1:-1]:
                offer(1, h, bit)
    for h in range(kv_heads):
        for slot in deeper:
            pass_on(1, h, slot)
    keys_all = n_sp * seq_rows
    score_scale = HEAD_WIDTH ** (-0.5)
    heads_done = []
    for kv in range(kv_heads):
        got_all(0, kv)
        keys = kbuf[kv].reshape(keys_all, HEAD_WIDTH)
        scores = (
            lax.dot_general(
                qs[kv], keys, (((1,), (1,)), ((), ())), preferred_element_type=jnp.float32
            )
            * score_scale
        )
        weights = jnp.exp(scores - jnp.max(scores, axis=-1, keepdims=True))
        total = jnp.sum(weights, axis=-1, keepdims=True)
        heads_done.append((weights.astype(jnp.bfloat16), total))
    for kv in range(kv_heads):
        got_all(1, kv)
        values = vbuf[kv].reshape(keys_all, HEAD_WIDTH)
        weights, total = heads_done[kv]
        mixed = jnp.dot(weights, values, preferred_element_type=jnp.float32) / total
        for member in range(groups):
            h = kv * groups + member
            att[:, h * HEAD_WIDTH : (h + 1) * HEAD_WIDTH] = mixed[
                member * seq_rows : (member + 1) * seq_rows
            ].astype(jnp.bfloat16)

    weight_copies[0].wait()
    def project(cols):
        product = (
            jnp.dot(att[...], ow[:, cols], preferred_element_type=jnp.float32)
            .astype(jnp.bfloat16)
            .reshape(n_y, 2, own, -1)
        )
        for core in range(2):
            part[core, :, :, cols] = product[:, core]

    def swap(j):
        cols = slice(j * tile, (j + 1) * tile)
        send(0, part.at[1 - c, :, :, cols], prx.at[:, :, cols], a_r.at[j], core_peer)

    project(slice(0, tile))
    cols = slice(0, tile)
    for dy in range(1, n_y):
        far = (y + dy) % n_y
        for core in range(2):
            send(
                0,
                part.at[(c + core) % 2, far, :, cols],
                direct.at[dy, core, :, :],
                g_r.at[dy - 1, core],
                (s, far * 2 + (c + core) % 2),
            )
    project(slice(tile, model))
    for j in range(1, tiles):
        swap(j)
    swap(0)
    for j in range(1, tiles):
        cols = slice(j * tile, (j + 1) * tile)
        arrive(prx.at[:, :, cols], a_r.at[j])
        for dy in range(1, n_y):
            far = (y + dy) % n_y
            psum[dy, :, cols] = (
                part[c, far, :, cols].astype(jnp.float32) + prx[far, :, cols].astype(jnp.float32)
            ).astype(jnp.bfloat16)
            send(
                0,
                psum.at[dy, :, cols],
                rsbuf.at[dy, :, cols],
                rs_r.at[j, dy - 1],
                (s, far * 2 + c),
            )
    arrive(prx.at[:, :, slice(0, tile)], a_r.at[0])
    inputs["x"].wait()
    inputs["fg"].wait()
    squares = jnp.zeros((own, 1), jnp.float32)
    for j in range(tiles):
        cols = slice(j * tile, (j + 1) * tile)
        summed = part[c, y, :, cols].astype(jnp.float32) + prx[y, :, cols].astype(jnp.float32)
        for dy in range(1, n_y):
            if j:
                arrive(rsbuf.at[dy, :, cols], rs_r.at[j, dy - 1])
                summed = summed + rsbuf[dy, :, cols].astype(jnp.float32)
            else:
                for core in range(2):
                    arrive(direct.at[dy, core, :, :], g_r.at[dy - 1, core])
                    summed = summed + direct[dy, core].astype(jnp.float32)
        middle = x_ref[:, cols].astype(jnp.float32) + summed.astype(jnp.bfloat16).astype(jnp.float32)
        mid[:, cols] = middle
        squares = squares + jnp.sum(middle * middle, axis=-1, keepdims=True)
    normed = (mid[...] * lax.rsqrt(squares / model + NORM_EPS) * fg_ref[...]).astype(jnp.bfloat16)
    chosen = (
        jnp.dot(picker, normed, preferred_element_type=jnp.float32)
        .astype(jnp.bfloat16)
        .reshape(n_sp, capacity, model)
    )
    disp[...] = chosen

    def dispatch(k):
        send(disp.at[k], rows.at[k, t], d_s.at[k], rows_r.at[k, t], (flip(s, order[k]), t))

    halves = [slice(i * model // 2, (i + 1) * model // 2) for i in range(2)]

    def dispatch(k):
        for i, cols in enumerate(halves):
            send(
                1,
                disp.at[k, :, cols],
                rows.at[k, c, y, :, cols],
                d_r.at[k, i],
                (flip(s, order[k]), t),
            )

    def forward(k):
        for i, cols in enumerate(halves):
            if k:
                arrive(rows.at[k, c, y, :, cols], d_r.at[k, i])
            for dy in range(1, n_y):
                peer = ((y + dy) % n_y) * 2 + c
                if k not in crossed:
                    send(
                        1,
                        rows.at[k, c, y, :, cols],
                        rows.at[k, c, y, :, cols],
                        y_r.at[k, (dy - 1) * 2 + i],
                        (s, peer),
                    )
            swap_rows(k, y, cols)

    def swap_rows(k, source, cols):
        group = sum(k >= edge for edge in edges[1:-1])
        send(
            1, rows.at[k, c, source, :, cols], rows.at[k, c, source, :, cols], c_r.at[group], core_peer
        )

    def relay(k):
        for dy in range(1, n_y):
            source = (y + n_y - dy) % n_y
            for i, cols in enumerate(halves):
                arrive(rows.at[k, c, source, :, cols], y_r.at[k, (dy - 1) * 2 + i])
                swap_rows(k, source, cols)

    def early(k):
        for dy in range(1, n_y):
            peer = ((y + dy) % n_y) * 2 + c
            send(1, disp.at[k], via.at[crossed.index(k), dy], v2_r.at[crossed.index(k), dy - 1], (s, peer))

    def onward(k):
        for dy in range(1, n_y):
            source = (y + n_y - dy) % n_y
            arrive(via.at[crossed.index(k), dy], v2_r.at[crossed.index(k), dy - 1])
            for i, cols in enumerate(halves):
                send(
                    1,
                    via.at[crossed.index(k), dy, :, cols],
                    rows.at[k, c, source, :, cols],
                    y_r.at[k, (dy - 1) * 2 + i],
                    (flip(s, order[k]), t),
                )

    def settle(g):
        arrive(rows.at[edges[g] : edges[g + 1], 1 - c], c_r.at[g])

    def span(g, j):
        return slice(edges[g], edges[g + 1]), slice(j * tile, (j + 1) * tile)

    def give_pair(g, j):
        ks, cols = span(g, j)
        send(2, eo.at[1 - c, :, ks, :, cols], cor.at[:, ks, :, cols], e_r.at[g, j], core_peer)

    def sum_pair(g, j):
        ks, cols = span(g, j)
        arrive(cor.at[:, ks, :, cols], e_r.at[g, j])
        for dy in range(1, n_y):
            far = (y + dy) % n_y
            pair[dy, ks, :, cols] = (
                eo[c, far, ks, :, cols].astype(jnp.float32) + cor[far, ks, :, cols].astype(jnp.float32)
            ).astype(jnp.bfloat16)
            send(
                2,
                pair.at[dy, ks, :, cols],
                yrec.at[dy, ks, :, cols],
                p_r.at[g * tiles + j, dy - 1],
                (s, far * 2 + c),
            )

    def give_back(g, j):
        ks, cols = span(g, j)
        whole = eo[c, y, ks, :, cols].astype(jnp.float32) + cor[y, ks, :, cols].astype(jnp.float32)
        for dy in range(1, n_y):
            arrive(yrec.at[dy, ks, :, cols], p_r.at[g * tiles + j, dy - 1])
            whole = whole + yrec[dy, ks, :, cols].astype(jnp.float32)
        res[ks, :, cols] = whole.astype(jnp.bfloat16)
        for k in range(edges[g], edges[g + 1]):
            if k:
                send(
                    2, res.at[k, :, cols], ret.at[k, :, cols], b_r.at[j], (flip(s, order[k]), t)
                )

    def run(hooks, name):
        do(*hooks.get(name, ()))

    def experts(g, hooks):
        low, high = edges[g], edges[g + 1]
        group_rows = (high - low) * n_tp * capacity
        block = rows[low:high].reshape(group_rows, model)
        f_tile = min(256, f_width)
        for j in range(f_width // f_tile):
            cols = slice(j * f_tile, (j + 1) * f_tile)
            gate = jnp.dot(block, wg[:, cols], preferred_element_type=jnp.float32)
            up = jnp.dot(block, wu[:, cols], preferred_element_type=jnp.float32)
            hid[:group_rows, cols] = (gate / (1.0 + jnp.exp(-gate)) * up).astype(jnp.bfloat16)
            run(hooks, f"gu{g}{j}")
        if g == 0:
            weight_copies[3].wait()
        for j in range(tiles):
            cols = slice(j * tile, (j + 1) * tile)
            down = jnp.dot(hid[:group_rows, :], wd[:, cols], preferred_element_type=jnp.float32)
            down = down.astype(jnp.bfloat16).reshape(high - low, 2, n_y, capacity, tile)
            for core in range(2):
                for far in range(n_y):
                    eo[core, far, low:high, :, cols] = down[:, core, far]
            give_pair(g, j)
            run(hooks, f"dn{g}{j}")

    steps = {"D": dispatch, "F": forward, "R": relay, "S": settle, "E": early, "V": onward, "P": sum_pair, "G": give_back}

    def do(*names):
        for name in names:
            steps[name[0]](*(int(d) for d in name[1:]))

    rows[0, c, y] = chosen[0]
    do("D2", "D3", "D1", "F0", "E4", "F1", "R0", "D5", "D6", "F2", "E7", "D4", "D7", "R1", "R2", "S0")
    weight_copies[1].wait()
    weight_copies[2].wait()
    experts(0, {"gu00": ("F3", "V4"), "gu01": ("V7",), "gu02": ("F5",), "dn00": ("R3", "F4"), "dn01": ("F6",), "dn03": ("R4", "P00")})
    do("R5", "P01", "S1", "P02", "P03")
    experts(1, {"gu13": ("R6", "F7"), "dn10": ("G00",), "dn11": ("R7",), "dn12": ("P10",), "dn13": ("P11", "G01")})
    do("S2")
    experts(2, {"gu20": ("P12", "G02", "P13"), "gu21": ("G03",), "gu23": ("G10",), "dn21": ("G11",), "dn22": ("P20",), "dn23": ("P21",)})
    do("P22", "G12", "P23", "G13", "G20", "G21", "G22", "G23")
    high = combiner.astype(jnp.bfloat16)
    rest = combiner - high.astype(jnp.float32)
    middle_part = rest.astype(jnp.bfloat16)
    low = (rest - middle_part.astype(jnp.float32)).astype(jnp.bfloat16)
    for j in range(tiles):
        cols = slice(j * tile, (j + 1) * tile)
        arrive(ret.at[1:, :, cols], b_r.at[j])
        returned = jnp.concatenate([res[0:1, :, cols], ret[1:, :, cols]]).reshape(total_slots, tile)
        routed = jnp.zeros((own, tile), jnp.float32)
        for piece in (high, middle_part, low):
            routed = routed + lax.dot_general(
                piece, returned, (((0,), (0,)), ((), ())), preferred_element_type=jnp.float32
            )
        out_ref[:, cols] = (mid[:, cols] + routed).astype(jnp.bfloat16)
    for stage, count in enumerate(sent):
        shipped = wg.at[pl.ds(0, count // f_width)]
        rdma(shipped, shipped, s_sem.at[stage], s_sem.at[stage], core_peer).wait_send()


def head_frequency():
    quarter = HEAD_WIDTH // 4
    frequency = ROPE_BASE ** (-np.arange(quarter, dtype=np.float32) / quarter)
    return jnp.asarray(np.tile(frequency, 4).reshape(1, HEAD_WIDTH), jnp.float32)


def local(
    x_resid,
    query_proj,
    projected_key_heads,
    projected_value_heads,
    query_gain,
    key_norm_gain,
    out_weight,
    ffn_gain,
    routing,
    route_scores,
    expert_gate,
    expert_up,
    expert_down,
):
    n_sp, n_tp = lax.axis_size("sp"), lax.axis_size("tp")
    own, model = x_resid.shape
    experts_all = n_sp * expert_gate.shape[0]
    capacity = max(2, 2 * own * TOP // experts_all)
    planned = (
        n_sp == PLAN_SPOTS
        and model == PLAN_TILES * min(512, model)
        and expert_gate.shape[2] == PLAN_TILES * min(256, expert_gate.shape[2])
    )
    if capacity % 16 or n_tp & (n_tp - 1) or n_tp < 2 or not planned or expert_gate.shape[0] != 1:
        return local_plain(
            x_resid,
            query_proj,
            projected_key_heads,
            projected_value_heads,
            query_gain,
            key_norm_gain,
            out_weight,
            ffn_gain,
            routing,
            route_scores,
            expert_gate,
            expert_up,
            expert_down,
        )
    seq_rows, q_width = query_proj.shape
    kv_width = projected_key_heads.shape[1]
    kv_heads = kv_width // HEAD_WIDTH
    groups = q_width // kv_width
    f_width = expert_gate.shape[2]
    n_y = n_tp // 2
    tiles = model // min(512, model)
    edges = group_edges(n_sp)
    groups_all = len(edges) - 1
    group_most = max(b - a for a, b in zip(edges, edges[1:]))
    bf16 = jnp.bfloat16
    dma = pltpu.SemaphoreType.DMA
    hbm = pl.BlockSpec(memory_space=pl.ANY)
    return pl.pallas_call(
        functools.partial(layer_kernel, n_sp, n_tp, capacity),
        out_shape=pltpu.VMEM((own, model), bf16),
        in_specs=[hbm] * 14,
        out_specs=pl.BlockSpec(memory_space=pltpu.VMEM),
        scratch_shapes=[
            pltpu.VMEM(query_proj.shape, bf16),
            pltpu.VMEM(projected_key_heads.shape, bf16),
            pltpu.VMEM((1, HEAD_WIDTH), jnp.float32),
            pltpu.VMEM((1, HEAD_WIDTH), jnp.float32),
            pltpu.VMEM((1, HEAD_WIDTH), jnp.float32),
            pltpu.VMEM((own, model), bf16),
            pltpu.VMEM((1, model), jnp.float32),
            pltpu.VMEM((TOP, own), jnp.int32),
            pltpu.VMEM((TOP, own), jnp.float32),
            pltpu.VMEM((kv_heads, n_sp, seq_rows, HEAD_WIDTH), bf16),
            pltpu.VMEM((kv_heads, n_sp, seq_rows, HEAD_WIDTH), bf16),
            pltpu.VMEM((kv_heads, groups * seq_rows, HEAD_WIDTH), bf16),
            pltpu.VMEM((seq_rows, q_width), bf16),
            pltpu.VMEM((2, n_y, own, model), bf16),
            pltpu.VMEM((n_y, own, model), bf16),
            pltpu.VMEM((n_y, own, model), bf16),
            pltpu.VMEM((n_y, own, model), bf16),
            pltpu.VMEM((n_y, 2, own, model // tiles), bf16),
            pltpu.VMEM((own, model), jnp.float32),
            pltpu.VMEM((n_sp, capacity, model), bf16),
            pltpu.VMEM((len(crossed_first(n_sp)), n_y, capacity, model), bf16),
            pltpu.VMEM((n_sp, 2, n_y, capacity, model), bf16),
            pltpu.VMEM((group_most * n_tp * capacity, f_width), bf16),
            pltpu.VMEM((2, n_y, n_sp, capacity, model), bf16),
            pltpu.VMEM((n_y, n_sp, capacity, model), bf16),
            pltpu.VMEM((n_y, n_sp, capacity, model), bf16),
            pltpu.VMEM((n_y, n_sp, capacity, model), bf16),
            pltpu.VMEM((n_sp, capacity, model), bf16),
            pltpu.VMEM((n_sp, capacity, model), bf16),
            pltpu.VMEM(out_weight.shape, bf16),
            pltpu.VMEM(expert_gate.shape[1:], bf16),
            pltpu.VMEM(expert_up.shape[1:], bf16),
            pltpu.VMEM(expert_down.shape[1:], bf16),
            dma((9 + kv_heads,)),
            dma((4,)),
            dma((3,)),
            dma((kv_heads, len(inner_slots(n_sp, 0)) + 1)),
            dma((kv_heads, len(inner_slots(n_sp, 1)) + 1)),
            dma((tiles,)),
            dma((tiles, n_y - 1)),
            dma((n_y - 1, 2)),
            dma((n_sp, 2)),
            dma((len(crossed_first(n_sp)), n_y - 1)),
            dma((n_sp, (n_y - 1) * 2)),
            dma((groups_all,)),
            dma((groups_all, tiles)),
            dma((groups_all * tiles, n_y - 1)),
            dma((tiles,)),
        ],
        compiler_params=pltpu.CompilerParams(
            collective_id=0, has_side_effects=True, vmem_limit_bytes=56 * 1024 * 1024
        ),
    )(
        query_proj,
        projected_key_heads,
        projected_value_heads,
        head_frequency(),
        query_gain.reshape(1, -1),
        key_norm_gain.reshape(1, -1),
        x_resid,
        ffn_gain.reshape(1, -1),
        routing.T,
        route_scores.T,
        out_weight,
        expert_gate,
        expert_up,
        expert_down,
    )


def solution(mesh):
    in_specs = (
        P(("sp", "tp"), None),
        P("sp", "tp"),
        P("sp", "tp"),
        P("sp", "tp"),
        P(),
        P(),
        P("tp", None),
        P(),
        P(("sp", "tp"), None),
        P(("sp", "tp"), None),
        P("sp", None, "tp"),
        P("sp", None, "tp"),
        P("sp", "tp", None),
    )
    out_specs = P(("sp", "tp"), None)
    return jax.shard_map(local, mesh=mesh, in_specs=in_specs, out_specs=out_specs, check_vma=False)
```
